32 devices in a mesh: sp: 8 (over z, core), tp: 4 (over y, x).
Axes of the slice: x: 2, y: 2, z: 4, core: 2. Of those that a mesh axis runs over, the one named last changes fastest.
Arguments:
- wide_queries: bfloat16 [512, 2560], P('sp', 'tp'), may hold values from -512 to 512
- narrow_queries: bfloat16 [512, 1536], P('sp', 'tp'), may hold values from -512 to 512
- kv_latent: bfloat16 [512, 512], P('sp'), may hold values from -6 to 6
- rope_key: bfloat16 [512, 32], P('sp'), may hold values from -4 to 4
- latent_gain: float32 [512], replicated, may hold values from 0.1 to 1.9
- wide_kv_weight: bfloat16 [512, 4096], P(None, 'tp'), may hold values from -0.25 to 0.25
- narrow_kv_weight: bfloat16 [512, 2048], P(None, 'tp'), may hold values from -0.25 to 0.25
- wide_out_weight: bfloat16 [2048, 2048], P('tp'), may hold values from -0.4375 to 0.4375
- narrow_out_weight: bfloat16 [1024, 2048], P('tp'), may hold values from -0.4375 to 0.4375
- residual: bfloat16 [512, 2048], P('sp'), may hold values from -6 to 6
- norm_gain: float32 [2048], replicated, may hold values from 0.1 to 1.9
- route_ids: int32 [512, 2], P('sp'), may hold values from 0 to 15, all different within a row; in each aligned block of 64 rows (0 to 63, 64 to 127, ...) at most 12 rows name the same one
- route_weights: float32 [512, 2], P('sp'), may hold values from 0.3 to 1.3
- expert_gate: bfloat16 [16, 2048, 1024], P('sp', None, 'tp'), may hold values from -0.125 to 0.125
- expert_up: bfloat16 [16, 2048, 1024], P('sp', None, 'tp'), may hold values from -0.125 to 0.125
- expert_down: bfloat16 [16, 1024, 2048], P('sp', 'tp'), may hold values from -0.1875 to 0.1875
- shared_gate: bfloat16 [2048, 1024], P(None, 'tp'), may hold values from -0.125 to 0.125
- shared_up: bfloat16 [2048, 1024], P(None, 'tp'), may hold values from -0.125 to 0.125
- shared_down: bfloat16 [1024, 2048], P('tp'), may hold values from -0.1875 to 0.1875
Outputs:
- mixed_out: bfloat16 [512, 2048], P('sp', 'tp')
The draws below stay inside these ranges and needn't reach their ends.
Inputs may be any that keep to these rules, and one draw needn't show every extreme that they name: `route_ids`: in the rows of one index of sp (aligned blocks of 64 rows) no expert is named by more than 12 rows, and some expert by exactly that many; each row names 2 different experts.
All inputs are finite; a program needn't handle non-finite values.
Results may differ from the reference program's by a relative error of at most 0.018.
Values may be sent and summed in bfloat16 or wider, within the bound.
A program may use at most 64 MiB of HBM per device.

```python
import math
import jax
import jax.numpy as jnp
import numpy as np
from jax import lax

D_MODEL = 2048
WIDE_HEADS = 16
NARROW_HEADS = 16
WIDE_NOPE = 128
WIDE_VALUE = 128
NARROW_NOPE = 64
NARROW_VALUE = 64
ROPE_DIM = 32
LATENT = 512
EXPERT_FF = 1024
TOP_K = 2
TOK_DEV = 64
TOKENS = 512
EXPERTS = 16
CAPACITY = 12
N_SP = 8
N_TP = 4


def queries_for(key, head_count, nope_width, salt):
    full_width = nope_width + ROPE_DIM
    base = 2.0 * jax.random.normal(jax.random.fold_in(key, salt), (TOKENS, head_count, full_width), jnp.float32)
    base = jnp.clip(base, -12.0, 12.0)
    return base.reshape(TOKENS, head_count * full_width).astype(jnp.bfloat16)


def draw_wide_queries(key, part):
    return queries_for(key, WIDE_HEADS, WIDE_NOPE, 31)


def draw_narrow_queries(key, part):
    return queries_for(key, NARROW_HEADS, NARROW_NOPE, 32)


def draw_rope_key(key, part):
    base = jnp.clip(jax.random.normal(jax.random.fold_in(key, 21), (TOKENS, ROPE_DIM), jnp.float32), -4.0, 4.0)
    return base.astype(jnp.bfloat16)


def shard_levels(rng, shape, split, least, top_value):
    loudness, own = 1.0, jax.random.fold_in(rng, 6)
    for axis_at, blocks in split:
        draws = jnp.exp(jax.random.uniform(jax.random.fold_in(own, axis_at), (blocks,), jnp.float32, least / len(split), top_value / len(split)))
        loudness = loudness * jnp.repeat(draws, shape[axis_at] // blocks).reshape([-1 if axis == axis_at else 1 for axis in range(len(shape))])
    return loudness


def routed_block(own_key, own, number, rows, count, top, most, lean):
    ranking = jax.random.permutation(own_key, count)
    packed, usual = portions_of(count, rows * top, most, lean, True), portions_of(count, rows * top, most, lean, False)
    places = jnp.arange(count)

    def named(lengths, turn):
        used = int((lengths > 0).sum())
        fixed = max(1, used // 4)
        moved = fixed + (places - fixed + turn * (used - fixed)) % max(1, count - fixed)
        return jnp.zeros((count,), jnp.int32).at[ranking[jnp.where(places < fixed, places, moved)]].set(jnp.asarray(lengths, jnp.int32))

    lengths = jnp.where(number % 4 == 0, named(packed, number // 4), named(usual, number - number // 4 - 1))
    mixed = jax.random.permutation(jax.random.fold_in(own, 3), count)
    source_of, sink = mixed[0:count // 2 * 2:2], mixed[1:count // 2 * 2:2]
    room = jnp.minimum(lengths[source_of] - 1, most - lengths[sink]) // 2
    room = jnp.where((source_of == ranking[0]) | (sink == ranking[0]) | (lengths[sink] == 0), 0, jnp.maximum(room, 0))
    moved = jax.random.randint(jax.random.fold_in(own, 4), (count // 2,), 0, 1 << 20) % (room + 1)
    lengths = lengths.at[source_of].add(-moved).at[sink].add(moved)
    members = jnp.searchsorted(jnp.cumsum(lengths), jnp.arange(rows * top), side="right").astype(jnp.int32)
    table = members.reshape(top, rows).T
    table = table[jax.random.permutation(jax.random.fold_in(own, 1), rows)]
    turn = jax.random.randint(jax.random.fold_in(own, 2), (rows, 1), 0, top)
    return jnp.take_along_axis(table, (jnp.arange(top)[None, :] + turn) % top, axis=1)


def portions_of(count, total, reach, lean, full):
    portions = [(1 << 20) // math.isqrt(rank ** lean) + 1 for rank in range(1, count + 1)]
    largest = reach if full else min(reach, max(-(-total // count), total * portions[0] // sum(portions)))
    least = 1 if total - largest >= count - 1 else 0
    given, rest = [largest] + [least] * (count - 1), total - largest - least * (count - 1)
    while rest > 0:
        free = [i for i in range(1, count) if given[i] < largest] or [i for i in range(1, count) if given[i] < reach]
        mass, remaining = sum([portions[i] for i in free]), rest
        for i in free:
            addition = min(reach - given[i], max(1, remaining * portions[i] // mass), rest)
            given[i] = given[i] + addition
            rest = rest - addition
    return np.array(given)


def normal_values(rng, dims, scale, reach, split=(), kind=jnp.bfloat16):
    entries = scale * jax.random.normal(rng, dims, jnp.float32)
    if split:
        entries = entries * shard_levels(rng, dims, split, -0.22, 0.18)
    return jnp.clip(entries, -reach, reach).astype(kind)


def setup_inputs(seed: int = 0) -> dict:
    key_list = jax.random.split(jax.random.key(seed), 20)
    wide_queries = draw_wide_queries(jax.random.fold_in(key_list[19], 71), 0)
    narrow_queries = draw_narrow_queries(jax.random.fold_in(key_list[19], 71), 0)
    kv_latent = normal_values(key_list[2], (TOKENS, LATENT), 1.0, 6.0, ((0, 8),))
    rope_key = draw_rope_key(jax.random.fold_in(key_list[19], 71), 0)
    latent_gain = jnp.clip(1.0 + 0.18 * jax.random.normal(key_list[4], (LATENT,), jnp.float32), 0.1, 1.9)
    wide_kv_weight = normal_values(key_list[5], (LATENT, WIDE_HEADS * (WIDE_NOPE + WIDE_VALUE)), LATENT ** -0.5, 0.25, ((1, 4),))
    narrow_kv_weight = normal_values(key_list[6], (LATENT, NARROW_HEADS * (NARROW_NOPE + NARROW_VALUE)), LATENT ** -0.5, 0.25, ((1, 4),))
    wide_out_weight = normal_values(key_list[7], (WIDE_HEADS * WIDE_VALUE, D_MODEL), ((WIDE_HEADS * WIDE_VALUE + NARROW_HEADS * NARROW_VALUE) // 16) ** -0.5, 0.4375, ((0, 4),))
    narrow_out_weight = normal_values(key_list[8], (NARROW_HEADS * NARROW_VALUE, D_MODEL), ((WIDE_HEADS * WIDE_VALUE + NARROW_HEADS * NARROW_VALUE) // 16) ** -0.5, 0.4375, ((0, 4),))
    residual = normal_values(key_list[9], (TOKENS, D_MODEL), 1.0, 6.0, ((0, 8),))
    norm_gain = jnp.clip(1.0 + 0.18 * jax.random.normal(key_list[10], (D_MODEL,), jnp.float32), 0.1, 1.9)
    route_ids_keys = jax.random.split(jax.random.fold_in(key_list[11], 1), TOKENS // TOK_DEV)
    route_ids_turns = jax.random.permutation(jax.random.fold_in(key_list[11], 3), TOKENS // TOK_DEV)
    route_ids = jax.vmap(lambda own, number: routed_block(jax.random.fold_in(key_list[11], 2), own, number, TOK_DEV, EXPERTS, TOP_K, CAPACITY, 1))(route_ids_keys, route_ids_turns).reshape((TOKENS, TOP_K))
    route_weights = jnp.clip(0.3 + 0.99999994 * jax.random.uniform(key_list[12], (TOKENS, TOP_K), jnp.float32) ** shard_levels(key_list[12], (TOKENS, TOP_K), ((0, 8),), -0.2, 0.2), 0.3, 1.3)
    expert_gate = normal_values(key_list[13], (EXPERTS, D_MODEL, EXPERT_FF), D_MODEL ** -0.5, 0.125, ((0, 8), (2, 4)))
    expert_up = normal_values(key_list[14], (EXPERTS, D_MODEL, EXPERT_FF), D_MODEL ** -0.5, 0.125, ((0, 8), (2, 4)))
    expert_down = normal_values(key_list[15], (EXPERTS, EXPERT_FF, D_MODEL), EXPERT_FF ** -0.5, 0.1875, ((0, 8), (1, 4)))
    shared_gate = normal_values(key_list[16], (D_MODEL, EXPERT_FF), D_MODEL ** -0.5, 0.125, ((1, 4),))
    shared_up = normal_values(key_list[17], (D_MODEL, EXPERT_FF), D_MODEL ** -0.5, 0.125, ((1, 4),))
    shared_down = normal_values(key_list[18], (EXPERT_FF, D_MODEL), EXPERT_FF ** -0.5, 0.1875, ((0, 4),))
    return dict(wide_queries=wide_queries, narrow_queries=narrow_queries, kv_latent=kv_latent, rope_key=rope_key, latent_gain=latent_gain, wide_kv_weight=wide_kv_weight, narrow_kv_weight=narrow_kv_weight, wide_out_weight=wide_out_weight, narrow_out_weight=narrow_out_weight, residual=residual, norm_gain=norm_gain, route_ids=route_ids, route_weights=route_weights, expert_gate=expert_gate, expert_up=expert_up, expert_down=expert_down, shared_gate=shared_gate, shared_up=shared_up, shared_down=shared_down)


THETA = 10000.0
EPS = 1e-06

def stored(values):
    return lax.optimization_barrier(values.astype(jnp.bfloat16))

def rotate(values, positions):
    half_width = values.shape[-1] // 2
    frequency = THETA ** (-2.0 * jnp.arange(half_width, dtype=jnp.float32) / values.shape[-1])
    angles = positions.astype(jnp.float32)[:, None] * frequency[None, :]
    if values.ndim == 3:
        angles = angles[:, None, :]
    cosine = jnp.cos(angles)
    sine_part = jnp.sin(angles)
    as_float = values.astype(jnp.float32)
    first_half = as_float[..., :half_width]
    second_half = as_float[..., half_width:]
    return stored(jnp.concatenate([first_half * cosine - second_half * sine_part, second_half * cosine + first_half * sine_part], axis=-1))

def rms_scale(values, gain):
    as_float = values.astype(jnp.float32)
    scaled = as_float * lax.rsqrt(lax.optimization_barrier(jnp.mean(as_float * as_float, axis=-1, keepdims=True)) + EPS)
    return stored(scaled * gain)

def attend(queries, nope_width, key_nope, key_rot, values):
    token_count = queries.shape[0]
    scale = queries.shape[-1] ** (-0.5)
    query_nope = queries[..., :nope_width].astype(jnp.float32)
    query_rope = queries[..., nope_width:].astype(jnp.float32)
    keys_float = key_nope.astype(jnp.float32)
    rot_float = key_rot.astype(jnp.float32)
    values_float = values.astype(jnp.float32)
    key_pos = jnp.arange(token_count, dtype=jnp.int32)

    def one_block(block_index):
        first_row = (block_index * TOK_DEV).astype(jnp.int32)
        block_nope = lax.dynamic_slice_in_dim(query_nope, first_row, TOK_DEV, 0)
        block_rope = lax.dynamic_slice_in_dim(query_rope, first_row, TOK_DEV, 0)
        scores = jnp.einsum('qhd,khd->hqk', block_nope, keys_float)
        scores = (scores + jnp.einsum('qhr,kr->hqk', block_rope, rot_float)) * scale
        query_pos = first_row + jnp.arange(TOK_DEV, dtype=jnp.int32)
        allowed = (query_pos[:, None] >= key_pos[None, :])[None]
        scores = jnp.where(allowed, scores, -jnp.inf)
        row_peak = lax.optimization_barrier(jnp.max(scores, axis=-1, keepdims=True))
        expo = jnp.exp(scores - row_peak)
        row_total = lax.optimization_barrier(jnp.sum(expo, axis=-1))
        probs = stored(expo).astype(jnp.float32)
        mixed = jnp.einsum('hqk,khv->qhv', probs, values_float)
        return stored(mixed / row_total.T[:, :, None])
    blocks = lax.map(one_block, jnp.arange(token_count // TOK_DEV, dtype=jnp.int32))
    return blocks.reshape(token_count, queries.shape[1], values.shape[-1])

def reference(wide_queries, narrow_queries, kv_latent, rope_key, latent_gain, wide_kv_weight, narrow_kv_weight, wide_out_weight, narrow_out_weight, residual, norm_gain, route_ids, route_weights, expert_gate, expert_up, expert_down, shared_gate, shared_up, shared_down):
    token_count = residual.shape[0]
    positions = jnp.arange(token_count, dtype=jnp.int32)
    wide_q = wide_queries.reshape(token_count, WIDE_HEADS, WIDE_NOPE + ROPE_DIM)
    wide_q = jnp.concatenate([wide_q[..., :WIDE_NOPE], rotate(wide_q[..., WIDE_NOPE:], positions)], axis=-1)
    narrow_q = narrow_queries.reshape(token_count, NARROW_HEADS, NARROW_NOPE + ROPE_DIM)
    narrow_q = jnp.concatenate([narrow_q[..., :NARROW_NOPE], rotate(narrow_q[..., NARROW_NOPE:], positions)], axis=-1)
    key_rot = rotate(rope_key, positions)
    latent = rms_scale(kv_latent, latent_gain)
    wide_kv = stored(jnp.dot(latent, wide_kv_weight, preferred_element_type=jnp.float32))
    wide_kv = wide_kv.reshape(token_count, WIDE_HEADS, WIDE_NOPE + WIDE_VALUE)
    narrow_kv = stored(jnp.dot(latent, narrow_kv_weight, preferred_element_type=jnp.float32))
    narrow_kv = narrow_kv.reshape(token_count, NARROW_HEADS, NARROW_NOPE + NARROW_VALUE)
    wide_att = attend(wide_q, WIDE_NOPE, wide_kv[..., :WIDE_NOPE], key_rot, wide_kv[..., WIDE_NOPE:])
    narrow_att = attend(narrow_q, NARROW_NOPE, narrow_kv[..., :NARROW_NOPE], key_rot, narrow_kv[..., NARROW_NOPE:])
    wide_per = WIDE_HEADS // N_TP
    narrow_per = NARROW_HEADS // N_TP
    wide_proj = wide_out_weight.reshape(WIDE_HEADS, WIDE_VALUE, D_MODEL).astype(jnp.float32)
    narrow_proj = narrow_out_weight.reshape(NARROW_HEADS, NARROW_VALUE, D_MODEL).astype(jnp.float32)
    proj_total = jnp.zeros((token_count, D_MODEL), jnp.float32)
    for group_index in range(N_TP):
        wide_slice = slice(group_index * wide_per, (group_index + 1) * wide_per)
        narrow_slice = slice(group_index * narrow_per, (group_index + 1) * narrow_per)
        partial_sum = jnp.einsum('thv,hvd->td', wide_att[:, wide_slice].astype(jnp.float32), wide_proj[wide_slice])
        partial_sum = partial_sum + jnp.einsum('thv,hvd->td', narrow_att[:, narrow_slice].astype(jnp.float32), narrow_proj[narrow_slice])
        proj_total = proj_total + stored(partial_sum).astype(jnp.float32)
    attn_proj = stored(proj_total)
    stream = stored(residual.astype(jnp.float32) + attn_proj.astype(jnp.float32))
    normed = rms_scale(stream, norm_gain)
    unit_per = EXPERT_FF // N_TP
    shared_hidden = stored(jax.nn.silu(jnp.dot(normed, shared_gate, preferred_element_type=jnp.float32)) * jnp.dot(normed, shared_up, preferred_element_type=jnp.float32))
    shared_total = jnp.zeros((token_count, D_MODEL), jnp.float32)
    for group_index in range(N_TP):
        unit_slice = slice(group_index * unit_per, (group_index + 1) * unit_per)
        shared_total = shared_total + stored(jnp.dot(shared_hidden[:, unit_slice], shared_down[unit_slice], preferred_element_type=jnp.float32)).astype(jnp.float32)
    shared_out = stored(shared_total)
    flat_ids = route_ids.reshape(-1)
    flat_weights = route_weights.reshape(-1)
    copy_count = token_count * TOP_K
    slot_count = N_SP * CAPACITY

    def visit_expert(routed_acc, expert):
        picked = jnp.nonzero(flat_ids == expert, size=slot_count, fill_value=copy_count)[0].astype(jnp.int32)
        is_live = picked < copy_count
        safe_pick = jnp.minimum(picked, copy_count - 1).astype(jnp.int32)
        token_index = (safe_pick // TOP_K).astype(jnp.int32)
        picked_rows = normed[token_index]
        hidden_units = stored(jax.nn.silu(jnp.dot(picked_rows, expert_gate[expert], preferred_element_type=jnp.float32)) * jnp.dot(picked_rows, expert_up[expert], preferred_element_type=jnp.float32))
        down_weight = expert_down[expert]
        expert_total = jnp.zeros((slot_count, D_MODEL), jnp.float32)
        for group_index in range(N_TP):
            unit_slice = slice(group_index * unit_per, (group_index + 1) * unit_per)
            expert_total = expert_total + stored(jnp.dot(hidden_units[:, unit_slice], down_weight[unit_slice], preferred_element_type=jnp.float32)).astype(jnp.float32)
        expert_result = stored(expert_total).astype(jnp.float32)
        weighting = jnp.where(is_live, flat_weights[safe_pick], 0.0)
        routed_acc = routed_acc.at[token_index].add(weighting[:, None] * expert_result)
        return (routed_acc, None)
    routed, _ = lax.scan(visit_expert, jnp.zeros((token_count, D_MODEL), jnp.float32), jnp.arange(EXPERTS, dtype=jnp.int32))
    return (stream.astype(jnp.float32) + shared_out.astype(jnp.float32) + routed).astype(jnp.bfloat16)
```

```python
import functools
import math

import jax
import jax.numpy as jnp
from jax import lax
from jax.experimental import pallas as pl
from jax.experimental.pallas import tpu as pltpu
from jax.sharding import PartitionSpec as P

MESH = pl.DeviceIdType.MESH
WIDE_NOPE = 128
WIDE_VALUE = 128
NARROW_NOPE = 64
NARROW_VALUE = 64
ROPE_DIM = 32
LANES = 128

THETA = 10000.0
EPS = 1e-06
FLOOR = -1e30
F32 = jnp.float32
BF16 = jnp.bfloat16


def dot(a, b):
    return jnp.dot(a, b, preferred_element_type=F32)


def dot_t(a, b):
    return lax.dot_general(a, b, (((1,), (1,)), ((), ())), preferred_element_type=F32)


def one_hot(cond):
    return jnp.where(cond, 1.0, 0.0).astype(BF16)


def silu(v):
    return v / (1.0 + jnp.exp(-v))


def aligned_queries(queries, nope, heads, cosine, sine):
    rows, full = queries.shape[1], nope + ROPE_DIM

    def grid(width):
        shape = (rows, width)
        return lax.broadcasted_iota(jnp.int32, shape, 0), lax.broadcasted_iota(jnp.int32, shape, 1)

    i, j = grid(heads * LANES)
    d = j & (LANES - 1)
    plain = one_hot((i == (j >> 7) * full + d) & (d < nope))
    i, j = grid(LANES)
    start = (j >> 5) * full + nope
    d = j & (ROPE_DIM - 1)
    straight = one_hot(i == start + d)
    swapped = one_hot(i == start + (d ^ (ROPE_DIM // 2)))
    moved = dot(queries, plain).astype(BF16)
    turned = (dot(queries, straight) * cosine + dot(queries, swapped) * sine).astype(BF16)
    return moved, turned


def kernel(
    dims,
    wq_ref, nq_ref, kv_ref, rope_ref, lgain_ref, res_ref, ngain_ref, ids_ref, idst_ref, rw_ref,
    cos_ref, sin_ref, rowe_ref, rowc_ref, cole_ref, colc_ref,
    wkv_hbm, nkv_hbm, wout_hbm, nout_hbm, gate_hbm, up_hbm, down_hbm, sg_hbm, su_hbm, sd_hbm,
    out_ref,
    wkv, nkv, wout, nout, gate, up, down, sg, su, sd,
    blk, kv_all, part, part_in, strm, nrm, disp, arr, acc, shp, sh_in, pd, pd_in, ret, back,
    load_sem, ag_send, fw_send, ag_recv, p_send, p_recv, st_send, st_recv,
    di_send, rl_send, ar_recv, sh_send, sh_recv, pd_send, pd_recv, rt_send, rt_recv,
):
    S, T, R, cap = dims
    s, t = lax.axis_index("sp"), lax.axis_index("tp")
    core, z, nz = lax.rem(s, 2), s // 2, S // 2
    sib = s + 1 - 2 * core
    tok = kv_ref.shape[0]
    latent_dim = kv_ref.shape[1]
    CW = out_ref.shape[1]
    D = res_ref.shape[1]

    def rc(src, dst, ss, rs, sp, tp):
        return pltpu.make_async_remote_copy(
            src_ref=src, dst_ref=dst, send_sem=ss, recv_sem=rs, device_id=(sp, tp), device_id_type=MESH
        )

    def sp_at(d):
        return lax.rem(s + d, S)

    def tp_at(d):
        return lax.rem(t + d, T)

    def each(lo, hi, body):
        lax.fori_loop(lo, hi, lambda i, carry: (body(i), carry)[1], 0)

    loads = [
        pltpu.make_async_copy(src, dst, load_sem.at[i])
        for i, (src, dst) in enumerate(
            [
                (wkv_hbm, wkv), (nkv_hbm, nkv), (wout_hbm, wout), (nout_hbm, nout), (sg_hbm, sg),
                (su_hbm, su), (sd_hbm, sd), (gate_hbm, gate), (up_hbm, up), (down_hbm, down),
            ]
        )
    ]

    barrier = pltpu.get_barrier_semaphore()

    def greet_sp(d):
        pl.semaphore_signal(barrier, inc=1, device_id=(sp_at(d), t), device_id_type=MESH)

    def greet_tp(d):
        pl.semaphore_signal(barrier, inc=1, device_id=(s, tp_at(d)), device_id_type=MESH)

    each(1, S, greet_sp)
    each(1, T, greet_tp)
    for load in loads:
        load.start()

    cosine, sine = cos_ref[...], sin_ref[...]
    lat = kv_ref[...].astype(F32)
    lat = lat * lax.rsqrt(jnp.mean(lat * lat, axis=-1, keepdims=True) + EPS)
    blk[:, :latent_dim] = (lat * lgain_ref[...]).astype(BF16)
    i = lax.broadcasted_iota(jnp.int32, (ROPE_DIM, LANES), 0)
    j = lax.broadcasted_iota(jnp.int32, (ROPE_DIM, LANES), 1) & (ROPE_DIM - 1)
    rope = rope_ref[...]
    key_rot = dot(rope, one_hot(i == j)) * cosine + dot(rope, one_hot(i == (j ^ (ROPE_DIM // 2)))) * sine
    blk[:, latent_dim:] = key_rot.astype(BF16)
    pl.semaphore_wait(barrier, S - 1 + T - 1)

    def ag_copy(d):
        target = 2 * lax.rem(z + d, nz) + core
        return rc(blk, kv_all.at[s], ag_send.at[d], ag_recv.at[s], target, t)

    def fw_copy(d):
        b = 2 * lax.rem(z + d, nz) + core
        return rc(kv_all.at[b], kv_all.at[b], fw_send.at[d], ag_recv.at[b], sib, t)

    own_copy = rc(blk, kv_all.at[s], ag_send.at[0], ag_recv.at[s], sib, t)
    each(1, nz, lambda d: ag_copy(d).start())
    own_copy.start()
    kv_all[s] = blk[...]

    wide_heads = wq_ref.shape[1] // (WIDE_NOPE + ROPE_DIM)
    narrow_heads = nq_ref.shape[1] // (NARROW_NOPE + ROPE_DIM)
    wq, wr = aligned_queries(wq_ref[...], WIDE_NOPE, wide_heads, cosine, sine)
    nq, nr = aligned_queries(nq_ref[...], NARROW_NOPE, narrow_heads, cosine, sine)

    ii = lax.broadcasted_iota(jnp.int32, (tok, tok), 0)
    jj = lax.broadcasted_iota(jnp.int32, (tok, tok), 1)
    top = ids_ref.shape[1]
    hit_t = [ids_ref[:, k : k + 1] == rowe_ref[...] for k in range(top)]
    rank_t = dot(one_hot(jj < ii), one_hot(functools.reduce(jnp.logical_or, hit_t)))
    picks = [one_hot(h & (rank_t == rowc_ref[...])) for h in hit_t]
    hit = functools.reduce(jnp.logical_or, [cole_ref[...] == idst_ref[k : k + 1, :] for k in range(top)])
    spread = one_hot(hit & (dot(one_hot(hit), one_hot(ii < jj)) == colc_ref[...]))

    def relay_key(d):
        copy = fw_copy(nz - d)
        copy.wait_recv()
        copy.start()

    each(1, nz, relay_key)

    def rest_of_keys(d):
        b = 2 * lax.rem(z + d, nz) + 1 - core
        rc(blk, kv_all.at[b], ag_send.at[0], ag_recv.at[b], sib, t).wait_recv()

    each(0, nz, rest_of_keys)

    keys = S * tok
    latents = kv_all[:, :, :latent_dim].reshape(keys, latent_dim)
    kr = kv_all[:, :, latent_dim:].reshape(keys, LANES)
    query_pos = lax.broadcasted_iota(jnp.int32, (tok, keys), 0) + s * tok
    allowed = query_pos >= lax.broadcasted_iota(jnp.int32, (tok, keys), 1)
    lane = lax.broadcasted_iota(jnp.int32, (tok, LANES), 1)

    def attend(moved, turned, h, keys_h, values_h, width):
        rot = jnp.where((lane >> 5) == h, turned.astype(F32), 0.0).astype(BF16)
        query = jnp.concatenate([moved[:, h * LANES : (h + 1) * LANES], rot], axis=1)
        scores = dot_t(query, jnp.concatenate([keys_h, kr], axis=1)) * width ** (-0.5)
        scores = jnp.where(allowed, scores, FLOOR)
        weights = jnp.exp(scores - jnp.max(scores, axis=-1, keepdims=True))
        total = jnp.sum(weights, axis=-1, keepdims=True)
        return dot(weights.astype(BF16), values_h) / total

    loads[0].wait()
    attended = []
    for h in range(wide_heads):
        kv = dot(latents, wkv[:, h * 2 * LANES : (h + 1) * 2 * LANES]).astype(BF16)
        attended.append(
            attend(wq, wr, h, kv[:, :LANES], kv[:, LANES:], WIDE_NOPE + ROPE_DIM).astype(BF16)
        )
    loads[1].wait()
    narrow = []
    for h in range(narrow_heads):
        kv = dot(latents, nkv[:, h * LANES : (h + 1) * LANES]).astype(BF16)
        narrow.append(attend(nq, nr, h, kv, kv, NARROW_NOPE + ROPE_DIM))
    n_att = []
    for h in range(0, narrow_heads, 2):
        first = pltpu.roll(narrow[h], NARROW_VALUE, 1)
        if h + 1 < narrow_heads:
            n_att.append(jnp.where(lane < NARROW_VALUE, first, narrow[h + 1]).astype(BF16))
        else:
            n_att.append(first[:, :NARROW_VALUE].astype(BF16))
    w_att = jnp.concatenate(attended, axis=1) if wide_heads > 1 else attended[0]
    n_att = jnp.concatenate(n_att, axis=1) if len(n_att) > 1 else n_att[0]

    def columns(d):
        return pl.ds(pl.multiple_of(d * CW, CW), CW)

    loads[2].wait()
    loads[3].wait()

    def p_copy(d):
        tt = tp_at(d)
        return rc(part.at[tt], part_in.at[t], p_send.at[d], p_recv.at[t], s, tt)

    def project(d):
        tt = tp_at(d)
        part[tt] = (dot(w_att, wout[:, columns(tt)]) + dot(n_att, nout[:, columns(tt)])).astype(BF16)

    def project_and_send(d):
        project(d)
        p_copy(d).start()

    each(1, T, project_and_send)
    project(0)
    total = part[t].astype(F32)
    for d in range(1, T):
        tt = tp_at(d)
        rc(part.at[t], part_in.at[tt], p_send.at[d], p_recv.at[tt], s, tt).wait_recv()
        total = total + part_in[tt].astype(F32)
    strm[t] = (res_ref[:, columns(t)].astype(F32) + total.astype(BF16).astype(F32)).astype(BF16)

    def st_copy(d):
        return rc(strm.at[t], strm.at[t], st_send.at[d], st_recv.at[t], s, tp_at(d))

    each(1, T, lambda d: st_copy(d).start())
    own = strm[t].astype(F32)
    square = jnp.sum(own * own, axis=-1, keepdims=True)
    for d in range(1, T):
        tt = tp_at(d)
        rc(strm.at[t], strm.at[tt], st_send.at[d], st_recv.at[tt], s, tt).wait_recv()
        theirs = strm[tt].astype(F32)
        square = square + jnp.sum(theirs * theirs, axis=-1, keepdims=True)
    scale = lax.rsqrt(square / D + EPS)
    own_normed = (own * scale * ngain_ref[:, columns(t)]).astype(BF16)

    disp[...] = dot(spread, own_normed).reshape(S, R, CW).astype(BF16)

    def di_copy(d):
        to = lax.rem(s + S - d, S)
        return rc(disp.at[to], arr.at[t, s], di_send.at[d], ar_recv.at[t, s], to, t)

    def rl_own(d):
        return rc(disp.at[s], arr.at[t, s], rl_send.at[0, d], ar_recv.at[t, s], s, tp_at(d))

    each(1, S, lambda d: di_copy(d).start())
    each(1, T, lambda d: rl_own(d).start())
    arr[t, s] = disp[s]
    for tt in range(T):
        nrm[:, tt * CW : (tt + 1) * CW] = (
            strm[tt].astype(F32) * scale * ngain_ref[:, tt * CW : (tt + 1) * CW]
        ).astype(BF16)

    for i in range(4, 7):
        loads[i].wait()
    normed = nrm[...]
    hidden = (silu(dot(normed, sg[...])) * dot(normed, su[...])).astype(BF16)

    def sh_copy(d):
        tt = tp_at(d)
        return rc(shp.at[tt], sh_in.at[t], sh_send.at[d], sh_recv.at[t], s, tt)

    def shared_columns(d):
        tt = tp_at(d)
        shp[tt] = dot(hidden, sd[:, columns(tt)]).astype(BF16)

    def rl_copy(d, e):
        b = sp_at(d)
        return rc(arr.at[t, b], arr.at[t, b], rl_send.at[d, e], ar_recv.at[t, b], s, tp_at(e))

    def relay_rows(d):
        b = sp_at(d)
        rc(disp.at[s], arr.at[t, b], di_send.at[d], ar_recv.at[t, b], b, t).wait_recv()
        each(1, T, lambda e: rl_copy(d, e).start())

    each(1, S, relay_rows)

    def shared_and_send(d):
        shared_columns(d)
        sh_copy(d).start()

    each(1, T, shared_and_send)
    shared_columns(0)

    for i in range(7, 10):
        loads[i].wait()
    local_experts = gate.shape[0]
    acc[...] = jnp.zeros_like(acc)

    def expert_chunk(d):
        tt = tp_at(d)
        rows = arr[tt].astype(F32).reshape(S * R, CW).astype(BF16)
        for e in range(local_experts):
            acc[2 * e] += dot(rows, gate[e, columns(tt), :])
            acc[2 * e + 1] += dot(rows, up[e, columns(tt), :])

    def arrived_chunk(d):
        tt = tp_at(d)

        def arrived(b):
            rc(disp.at[s], arr.at[tt, b], rl_send.at[0, d], ar_recv.at[tt, b], s, tt).wait_recv()

        each(0, S, arrived)
        expert_chunk(d)

    expert_chunk(0)
    each(1, T, arrived_chunk)
    slot_expert = cole_ref[...]
    units = []
    for e in range(local_experts):
        value = silu(acc[2 * e]) * acc[2 * e + 1]
        mine = functools.reduce(
            jnp.logical_or, [slot_expert == b * local_experts + e for b in range(S)]
        )
        units.append(jnp.where(mine, value, 0.0).astype(BF16))

    def pd_copy(d, i):
        tt, b = tp_at(d), sp_at(i)
        return rc(pd.at[tt, b], pd_in.at[t, b], pd_send.at[d, i], pd_recv.at[t, b], s, tt)

    def down_columns(d):
        tt = tp_at(d)
        value = dot(units[0], down[0, :, columns(tt)])
        for e in range(1, local_experts):
            value = value + dot(units[e], down[e, :, columns(tt)])
        pd[tt] = value.reshape(S, R, CW).astype(BF16)

    def down_and_send(d):
        down_columns(d)
        each(1, S + 1, lambda i: pd_copy(d, lax.rem(i, S)).start())

    each(1, T, down_and_send)
    down_columns(0)

    shared = shp[t].astype(F32)
    for d in range(1, T):
        tt = tp_at(d)
        rc(shp.at[t], sh_in.at[tt], sh_send.at[d], sh_recv.at[tt], s, tt).wait_recv()
        shared = shared + sh_in[tt].astype(F32)
    base = strm[t].astype(F32) + shared.astype(BF16).astype(F32)

    def summed(b):
        value = pd[t, b].astype(F32)
        for d in range(1, T):
            tt = tp_at(d)
            rc(pd.at[t, b], pd_in.at[tt, b], pd_send.at[d, 0], pd_recv.at[tt, b], s, tt).wait_recv()
            value = value + pd_in[tt, b].astype(F32)
        return value.astype(BF16)

    def rt_copy(d):
        b = sp_at(d)
        return rc(ret.at[b], back.at[s], rt_send.at[d], rt_recv.at[s], b, t)

    def send_back(d):
        b = sp_at(d)
        ret[b] = summed(b)
        rt_copy(d).start()

    each(1, S, send_back)
    back[s] = summed(s)

    def returned(d):
        b = sp_at(d)
        rc(ret.at[s], back.at[b], rt_send.at[d], rt_recv.at[b], b, t).wait_recv()

    each(1, S, returned)
    rows = back[...].astype(F32).reshape(S * R, CW).astype(BF16)
    for k in range(top):
        base = base + dot(picks[k], rows) * rw_ref[:, k : k + 1]
    out_ref[...] = base.astype(BF16)

    own_copy.wait_send()
    each(1, nz, lambda d: ag_copy(d).wait_send())
    each(1, nz, lambda d: fw_copy(d).wait_send())
    each(1, S, lambda d: di_copy(d).wait_send())
    each(1, S, lambda d: rt_copy(d).wait_send())

    def close(e):
        p_copy(e).wait_send()
        st_copy(e).wait_send()
        sh_copy(e).wait_send()
        rl_own(e).wait_send()
        each(1, S, lambda d: rl_copy(d, e).wait_send())
        each(0, S, lambda i: pd_copy(e, i).wait_send())

    each(1, T, close)


def local(
    S, T,
    wide_queries, narrow_queries, kv_latent, rope_key, latent_gain, wide_kv_weight, narrow_kv_weight,
    wide_out_weight, narrow_out_weight, residual, norm_gain, route_ids, route_weights,
    expert_gate, expert_up, expert_down, shared_gate, shared_up, shared_down,
):
    tok, D = residual.shape
    latent_dim = kv_latent.shape[1]
    top = route_ids.shape[1]
    local_experts = expert_gate.shape[0]
    cap = max(2, 3 * tok * top // (2 * S * local_experts))
    R = -(-local_experts * cap // 8) * 8
    CW = D // T

    half = ROPE_DIM // 2
    positions = (lax.axis_index("sp") * tok + jnp.arange(tok, dtype=jnp.int32)).astype(F32)
    lane = jnp.arange(LANES, dtype=jnp.int32)
    frequency = THETA ** (-2.0 * (lane % half).astype(F32) / ROPE_DIM)
    angles = positions[:, None] * frequency[None, :]
    cosine = jnp.cos(angles)
    sine = jnp.where((lane % ROPE_DIM < half)[None, :], -1.0, 1.0) * jnp.sin(angles)

    slot = jnp.arange(S * R, dtype=jnp.int32)
    within = slot % R
    slot_expert = jnp.where(
        within < local_experts * cap, slot // R * local_experts + within // cap, -1
    ).astype(jnp.int32)
    slot_place = (within % cap).astype(F32)

    vm = pl.BlockSpec(memory_space=pltpu.VMEM)
    hbm = pl.BlockSpec(memory_space=pl.ANY)
    weights = (
        wide_kv_weight, narrow_kv_weight, wide_out_weight, narrow_out_weight,
        expert_gate, expert_up, expert_down, shared_gate, shared_up, shared_down,
    )
    small = (
        wide_queries, narrow_queries, kv_latent, rope_key, latent_gain[None, :], residual,
        norm_gain[None, :], route_ids, route_ids.T, route_weights, cosine, sine,
        slot_expert[None, :], slot_place[None, :], slot_expert[:, None], slot_place[:, None],
    )
    V = pltpu.VMEM
    sem = pltpu.SemaphoreType.DMA
    ff = expert_gate.shape[2]
    scratch = [V(w.shape, w.dtype) for w in weights] + [
        V((tok, latent_dim + LANES), BF16),
        V((S, tok, latent_dim + LANES), BF16),
        V((T, tok, CW), BF16),
        V((T, tok, CW), BF16),
        V((T, tok, CW), BF16),
        V((tok, D), BF16),
        V((S, R, CW), BF16),
        V((T, S, R, CW), BF16),
        V((2 * local_experts, S * R, ff), F32),
        V((T, tok, CW), BF16),
        V((T, tok, CW), BF16),
        V((T, S, R, CW), BF16),
        V((T, S, R, CW), BF16),
        V((S, R, CW), BF16),
        V((S, R, CW), BF16),
        sem((len(weights),)), sem((S // 2,)), sem((S // 2,)), sem((S,)),
        sem((T,)), sem((T,)), sem((T,)), sem((T,)),
        sem((S,)), sem((S, T)), sem((T, S)), sem((T,)), sem((T,)),
        sem((T, S)), sem((T, S)), sem((S,)), sem((S,)),
    ]
    return pl.pallas_call(
        functools.partial(kernel, (S, T, R, cap)),
        out_shape=jax.ShapeDtypeStruct((tok, CW), BF16),
        in_specs=[vm] * len(small) + [hbm] * len(weights),
        out_specs=vm,
        scratch_shapes=scratch,
        compiler_params=pltpu.CompilerParams(
            collective_id=0, has_side_effects=True, vmem_limit_bytes=60 * 1024 * 1024
        ),
    )(*small, *weights)


def solution(mesh):
    placed = (
        P("sp", "tp"),
        P("sp", "tp"),
        P("sp", None),
        P("sp", None),
        P(),
        P(None, "tp"),
        P(None, "tp"),
        P("tp", None),
        P("tp", None),
        P("sp", None),
        P(),
        P("sp", None),
        P("sp", None),
        P("sp", None, "tp"),
        P("sp", None, "tp"),
        P("sp", "tp", None),
        P(None, "tp"),
        P(None, "tp"),
        P("tp", None),
    )
    return jax.shard_map(
        functools.partial(local, mesh.shape["sp"], mesh.shape["tp"]),
        mesh=mesh, in_specs=placed, out_specs=P("sp", "tp"), check_vma=False,
    )
```

```python
import functools
import math

import jax
import jax.numpy as jnp
from jax import lax
from jax.experimental import pallas as pl
from jax.experimental.pallas import tpu as pltpu
from jax.sharding import PartitionSpec as P

MESH = pl.DeviceIdType.MESH
WIDE_NOPE = 128
WIDE_VALUE = 128
NARROW_NOPE = 64
NARROW_VALUE = 64
ROPE_DIM = 32
LANES = 128

THETA = 10000.0
EPS = 1e-06
FLOOR = -1e30
F32 = jnp.float32
BF16 = jnp.bfloat16


def dot(a, b):
    return jnp.dot(a, b, preferred_element_type=F32)


def dot_t(a, b):
    return lax.dot_general(a, b, (((1,), (1,)), ((), ())), preferred_element_type=F32)


def one_hot(cond):
    return jnp.where(cond, 1.0, 0.0).astype(BF16)


def silu(v):
    return v / (1.0 + jnp.exp(-v))


def aligned_queries(queries, nope, heads, cosine, sine):
    rows, full = queries.shape[1], nope + ROPE_DIM

    def grid(width):
        shape = (rows, width)
        return lax.broadcasted_iota(jnp.int32, shape, 0), lax.broadcasted_iota(jnp.int32, shape, 1)

    i, j = grid(heads * LANES)
    d = j & (LANES - 1)
    plain = one_hot((i == (j >> 7) * full + d) & (d < nope))
    i, j = grid(LANES)
    start = (j >> 5) * full + nope
    d = j & (ROPE_DIM - 1)
    straight = one_hot(i == start + d)
    swapped = one_hot(i == start + (d ^ (ROPE_DIM // 2)))
    moved = dot(queries, plain).astype(BF16)
    turned = (dot(queries, straight) * cosine + dot(queries, swapped) * sine).astype(BF16)
    return moved, turned


def kernel(
    dims,
    wq_ref, nq_ref, kv_ref, ropet_ref, lgain_ref, res_ref, ngain_ref, idst_ref, rwt_ref,
    wkv_hbm, nkv_hbm, wout_hbm, nout_hbm, gate_hbm, up_hbm, down_hbm, sg_hbm, su_hbm, sd_hbm,
    out_ref,
    wkv, nkv, wout, nout, gate, up, down, sg, su, sd,
    blk, rot, kv_all, rot_all, part, part_in, strm, disp, arr, acc, shp, sh_in, pd, pd_in, ret, back,
    load_sem, ag_send, fw_send, ag_recv, p_send, p_recv, st_send, st_recv,
    di_send, rl_send, ar_recv, sh_send, sh_recv, pd_send, pd_recv, rt_send, rt_recv,
):
    S, T, R, cap = dims
    s, t = lax.axis_index("sp"), lax.axis_index("tp")
    core, z, nz = lax.rem(s, 2), s // 2, S // 2
    sib = s + 1 - 2 * core
    tok = kv_ref.shape[0]
    latent_dim = kv_ref.shape[1]
    CW = out_ref.shape[1]
    D = res_ref.shape[1]

    def rc(src, dst, ss, rs, sp, tp):
        return pltpu.make_async_remote_copy(
            src_ref=src, dst_ref=dst, send_sem=ss, recv_sem=rs, device_id=(sp, tp), device_id_type=MESH
        )

    def sp_at(d):
        return lax.rem(s + d, S)

    def tp_at(d):
        if T == 4:
            return 2 * lax.rem(t // 2 + (4 - d) // 2, 2) + lax.rem(t + d, 2)
        return lax.rem(t + d, T)

    def each(lo, hi, body):
        lax.fori_loop(lo, hi, lambda i, carry: (body(i), carry)[1], 0)

    loads = [
        pltpu.make_async_copy(src, dst, load_sem.at[i])
        for i, (src, dst) in enumerate(
            [
                (wkv_hbm, wkv), (nkv_hbm, nkv), (wout_hbm, wout), (nout_hbm, nout), (sg_hbm, sg),
                (su_hbm, su), (sd_hbm, sd), (gate_hbm, gate), (up_hbm, up), (down_hbm, down),
            ]
        )
    ]

    barrier = pltpu.get_barrier_semaphore()

    def greet_sp(d):
        pl.semaphore_signal(barrier, inc=1, device_id=(sp_at(d), t), device_id_type=MESH)

    def greet_tp(d):
        pl.semaphore_signal(barrier, inc=1, device_id=(s, tp_at(d)), device_id_type=MESH)

    each(1, S, greet_sp)
    each(1, T, greet_tp)
    for load in loads:
        load.start()

    half = ROPE_DIM // 2
    lane = lax.broadcasted_iota(jnp.int32, (tok, LANES), 1)
    row = lax.broadcasted_iota(jnp.int32, (tok, LANES), 0)
    frequency = jnp.zeros((tok, LANES), F32)
    for n in range(half):
        frequency = jnp.where((lane & (half - 1)) == n, float(THETA ** (-2.0 * n / ROPE_DIM)), frequency)
    angles = (s * tok + row).astype(F32) * frequency
    cosine = jnp.cos(angles)
    sine = jnp.where((lane & (ROPE_DIM - 1)) < half, -1.0, 1.0) * jnp.sin(angles)
    lat = kv_ref[...].astype(F32)
    lat = lat * lax.rsqrt(jnp.mean(lat * lat, axis=-1, keepdims=True) + EPS)
    blk[...] = (lat * lgain_ref[...]).astype(BF16)
    i = lax.broadcasted_iota(jnp.int32, (ROPE_DIM, LANES), 0)
    j = lax.broadcasted_iota(jnp.int32, (ROPE_DIM, LANES), 1) & (ROPE_DIM - 1)
    ii = lax.broadcasted_iota(jnp.int32, (tok, tok), 0)
    jj = lax.broadcasted_iota(jnp.int32, (tok, tok), 1)
    eye = one_hot(ii == jj)
    rope = dot_t(eye, ropet_ref[...]).astype(BF16)
    key_rot = dot(rope, one_hot(i == j)) * cosine + dot(rope, one_hot(i == (j ^ (ROPE_DIM // 2)))) * sine
    group = tok * ROPE_DIM // LANES
    lane_g = lax.broadcasted_iota(jnp.int32, (group, LANES), 1) // ROPE_DIM
    packed = key_rot[:group]
    for n in range(1, LANES // ROPE_DIM):
        packed = jnp.where(lane_g == n, key_rot[n * group : (n + 1) * group], packed)
    rot[...] = packed.astype(BF16)
    pl.semaphore_wait(barrier, S - 1 + T - 1)

    def ag_copies(d):
        target = 2 * lax.rem(z + d, nz) + core
        return (
            rc(blk, kv_all.at[s], ag_send.at[d], ag_recv.at[s], target, t),
            rc(rot, rot_all.at[s], ag_send.at[nz + d], ag_recv.at[S + s], target, t),
        )

    def fw_copies(d):
        b = 2 * lax.rem(z + d, nz) + core
        return (
            rc(kv_all.at[b], kv_all.at[b], fw_send.at[d], ag_recv.at[b], sib, t),
            rc(rot_all.at[b], rot_all.at[b], fw_send.at[nz + d], ag_recv.at[S + b], sib, t),
        )

    own_copies = (
        rc(blk, kv_all.at[s], ag_send.at[0], ag_recv.at[s], sib, t),
        rc(rot, rot_all.at[s], ag_send.at[nz], ag_recv.at[S + s], sib, t),
    )

    def start_keys(d):
        for copy in ag_copies(d):
            copy.start()

    each(1, nz, start_keys)
    for copy in own_copies:
        copy.start()
    kv_all[s] = blk[...]
    rot_all[s] = rot[...]

    wide_heads = wq_ref.shape[1] // (WIDE_NOPE + ROPE_DIM)
    narrow_heads = nq_ref.shape[1] // (NARROW_NOPE + ROPE_DIM)
    wq, wr = aligned_queries(wq_ref[...], WIDE_NOPE, wide_heads, cosine, sine)
    nq, nr = aligned_queries(nq_ref[...], NARROW_NOPE, narrow_heads, cosine, sine)

    top = idst_ref.shape[0]
    local_experts = gate.shape[0]

    def slots(width):
        slot = lax.broadcasted_iota(jnp.int32, (S * R, width), 0)
        block = sum((slot >= b * R).astype(jnp.int32) for b in range(1, S))
        within = slot - block * R
        inner = sum(((within >= e * cap).astype(jnp.int32) for e in range(1, local_experts)), jnp.zeros_like(slot))
        expert = jnp.where(within < local_experts * cap, block * local_experts + inner, -1)
        return inner, expert, (within - inner * cap).astype(F32)

    _, slot_expert, slot_place = slots(tok)
    hits = [slot_expert == idst_ref[k : k + 1, :] for k in range(top)]
    hit = functools.reduce(jnp.logical_or, hits)
    placed = dot(one_hot(hit), one_hot(ii < jj)) == slot_place
    spread = one_hot(hit & placed)
    picks = [dot_t(eye, one_hot(h & placed)).astype(BF16) for h in hits]
    own_weights = [
        jnp.sum(jnp.where(ii == jj, rwt_ref[k : k + 1, :], 0.0), axis=1, keepdims=True) for k in range(top)
    ]

    def relay_key(d):
        for copy in fw_copies(nz - d):
            copy.wait_recv()
            copy.start()

    each(1, nz, relay_key)

    def rest_of_keys(d):
        b = 2 * lax.rem(z + d, nz) + 1 - core
        rc(blk, kv_all.at[b], ag_send.at[0], ag_recv.at[b], sib, t).wait_recv()
        rc(rot, rot_all.at[b], ag_send.at[nz], ag_recv.at[S + b], sib, t).wait_recv()

    each(0, nz, rest_of_keys)

    keys = S * tok
    latents = kv_all[...].reshape(keys, latent_dim)
    packed = rot_all[...].reshape(S * group, LANES)
    i = lax.broadcasted_iota(jnp.int32, (LANES, LANES), 0)
    j = lax.broadcasted_iota(jnp.int32, (LANES, LANES), 1) & (ROPE_DIM - 1)
    kr = jnp.concatenate(
        [
            dot(packed, one_hot(i == n * ROPE_DIM + j)).astype(BF16).reshape(S, 1, group, LANES)
            for n in range(LANES // ROPE_DIM)
        ],
        axis=1,
    ).reshape(keys, LANES)
    query_pos = lax.broadcasted_iota(jnp.int32, (tok, keys), 0) + s * tok
    allowed = query_pos >= lax.broadcasted_iota(jnp.int32, (tok, keys), 1)

    def attend(moved, turned, h, keys_h, values_h, width):
        own_rot = jnp.where((lane >> 5) == h, turned.astype(F32), 0.0).astype(BF16)
        query = jnp.concatenate([moved[:, h * LANES : (h + 1) * LANES], own_rot], axis=1)
        scores = dot_t(query, jnp.concatenate([keys_h, kr], axis=1)) * width ** (-0.5)
        scores = jnp.where(allowed, scores, FLOOR)
        weights = jnp.exp(scores - jnp.max(scores, axis=-1, keepdims=True))
        total = jnp.sum(weights, axis=-1, keepdims=True)
        return dot(weights.astype(BF16), values_h) / total

    loads[0].wait()
    attended = []
    for h in range(wide_heads):
        kv = dot(latents, wkv[:, h * 2 * LANES : (h + 1) * 2 * LANES]).astype(BF16)
        attended.append(
            attend(wq, wr, h, kv[:, :LANES], kv[:, LANES:], WIDE_NOPE + ROPE_DIM).astype(BF16)
        )
    loads[1].wait()
    narrow = []
    for h in range(narrow_heads):
        kv = dot(latents, nkv[:, h * LANES : (h + 1) * LANES]).astype(BF16)
        narrow.append(attend(nq, nr, h, kv, kv, NARROW_NOPE + ROPE_DIM))
    n_att = []
    for h in range(0, narrow_heads, 2):
        first = pltpu.roll(narrow[h], NARROW_VALUE, 1)
        if h + 1 < narrow_heads:
            n_att.append(jnp.where(lane < NARROW_VALUE, first, narrow[h + 1]).astype(BF16))
        else:
            n_att.append(first[:, :NARROW_VALUE].astype(BF16))
    w_att = jnp.concatenate(attended, axis=1) if wide_heads > 1 else attended[0]
    n_att = jnp.concatenate(n_att, axis=1) if len(n_att) > 1 else n_att[0]

    def columns(d):
        return pl.ds(pl.multiple_of(d * CW, CW), CW)

    loads[2].wait()
    loads[3].wait()

    def p_copy(d):
        tt = tp_at(d)
        return rc(part.at[tt], part_in.at[t], p_send.at[d], p_recv.at[t], s, tt)

    def project_at(tt):
        part[tt] = (dot(w_att, wout[:, columns(tt)]) + dot(n_att, nout[:, columns(tt)])).astype(BF16)

    def project_and_send(d):
        project_at(tp_at(d))
        p_copy(d).start()

    each(1, T, project_and_send)
    project_at(t)
    total = part[t].astype(F32)
    for d in range(1, T):
        tt = tp_at(d)
        rc(part.at[t], part_in.at[tt], p_send.at[d], p_recv.at[tt], s, tt).wait_recv()
        total = total + part_in[tt].astype(F32)
    strm[t] = (res_ref[:, columns(t)].astype(F32) + total.astype(BF16).astype(F32)).astype(BF16)

    def st_copy(d):
        return rc(strm.at[t], strm.at[t], st_send.at[d], st_recv.at[t], s, tp_at(d))

    each(1, T, lambda d: st_copy(d).start())
    own = strm[t].astype(F32)
    square = jnp.sum(own * own, axis=-1, keepdims=True)
    for d in range(1, T):
        tt = tp_at(d)
        rc(strm.at[t], strm.at[tt], st_send.at[d], st_recv.at[tt], s, tt).wait_recv()
        theirs = strm[tt].astype(F32)
        square = square + jnp.sum(theirs * theirs, axis=-1, keepdims=True)
    scale = lax.rsqrt(square / D + EPS)
    own_normed = (own * scale * ngain_ref[:, columns(t)]).astype(BF16)

    disp[...] = dot(spread, own_normed).reshape(S, R, CW).astype(BF16)

    def di_copy(d):
        to = lax.rem(s + S - d, S)
        return rc(disp.at[to], arr.at[t, s], di_send.at[d], ar_recv.at[t, s], to, t)

    def rl_own(d):
        return rc(disp.at[s], arr.at[t, s], rl_send.at[0, d], ar_recv.at[t, s], s, tp_at(d))

    each(1, S, lambda d: di_copy(d).start())
    each(1, T, lambda d: rl_own(d).start())
    arr[t, s] = disp[s]
    for i in range(4, 7):
        loads[i].wait()

    def sh_copy(d):
        tt = tp_at(d)
        return rc(shp.at[tt], sh_in.at[t], sh_send.at[d], sh_recv.at[t], s, tt)

    def shared_columns(tt):
        shp[tt] = dot(hidden, sd[:, columns(tt)]).astype(BF16)

    def rl_copy(d, e):
        b = sp_at(d)
        return rc(arr.at[t, b], arr.at[t, b], rl_send.at[d, e], ar_recv.at[t, b], s, tp_at(e))

    def relay_rows(d):
        b = sp_at(d)
        rc(disp.at[s], arr.at[t, b], di_send.at[d], ar_recv.at[t, b], b, t).wait_recv()
        each(1, T, lambda e: rl_copy(d, e).start())

    acc[...] = jnp.zeros_like(acc)
    gated = jnp.zeros((tok, sg.shape[1]), F32)
    upped = jnp.zeros((tok, sg.shape[1]), F32)
    for n in range(T):
        chunk = (strm[n].astype(F32) * scale * ngain_ref[:, n * CW : (n + 1) * CW]).astype(BF16)
        gated += dot(chunk, sg[n * CW : (n + 1) * CW, :])
        upped += dot(chunk, su[n * CW : (n + 1) * CW, :])
        each(1 + (S - 1) * n // T, 1 + (S - 1) * (n + 1) // T, relay_rows)
    hidden = (silu(gated) * upped).astype(BF16)

    def shared_and_send(d):
        shared_columns(tp_at(d))
        sh_copy(d).start()

    each(1, T, shared_and_send)
    shared_columns(t)

    for i in range(7, 10):
        loads[i].wait()
    def expert_chunk(tt):
        rows = arr[tt].astype(F32).reshape(S * R, CW).astype(BF16)
        for e in range(local_experts):
            acc[2 * e] += dot(rows, gate[e, columns(tt), :])
            acc[2 * e + 1] += dot(rows, up[e, columns(tt), :])

    def arrived_chunk(d):
        tt = tp_at(d)

        def arrived(b):
            rc(disp.at[s], arr.at[tt, b], rl_send.at[0, d], ar_recv.at[tt, b], s, tt).wait_recv()

        each(0, S, arrived)
        expert_chunk(tt)

    expert_chunk(t)
    each(1, T, arrived_chunk)
    inner, _, _ = slots(gate.shape[2])
    units = []
    for e in range(local_experts):
        value = silu(acc[2 * e]) * acc[2 * e + 1]
        units.append(jnp.where(inner == e, value, 0.0).astype(BF16))

    def pd_copy(d, i):
        tt, b = tp_at(d), sp_at(i)
        return rc(pd.at[tt, b], pd_in.at[t, b], pd_send.at[d, i], pd_recv.at[t, b], s, tt)

    def down_columns(tt):
        value = dot(units[0], down[0, :, columns(tt)])
        for e in range(1, local_experts):
            value = value + dot(units[e], down[e, :, columns(tt)])
        pd[tt] = value.reshape(S, R, CW).astype(BF16)

    each(1, T, lambda d: down_columns(tp_at(d)))
    each(1, S + 1, lambda i: each(1, T, lambda d: pd_copy(d, lax.rem(i, S)).start()))
    down_columns(t)

    shared = shp[t].astype(F32)
    for d in range(1, T):
        tt = tp_at(d)
        rc(shp.at[t], sh_in.at[tt], sh_send.at[d], sh_recv.at[tt], s, tt).wait_recv()
        shared = shared + sh_in[tt].astype(F32)
    base = strm[t].astype(F32) + shared.astype(BF16).astype(F32)

    def summed(b):
        value = pd[t, b].astype(F32)
        for d in range(1, T):
            tt = tp_at(d)
            rc(pd.at[t, b], pd_in.at[tt, b], pd_send.at[d, 0], pd_recv.at[tt, b], s, tt).wait_recv()
            value = value + pd_in[tt, b].astype(F32)
        return value.astype(BF16)

    def rt_copy(d):
        b = sp_at(d)
        return rc(ret.at[b], back.at[s], rt_send.at[d], rt_recv.at[s], b, t)

    def send_back(d):
        b = sp_at(d)
        ret[b] = summed(b)
        rt_copy(d).start()

    each(1, S, send_back)
    back[s] = summed(s)

    def returned(d):
        b = sp_at(d)
        rc(ret.at[s], back.at[b], rt_send.at[d], rt_recv.at[b], b, t).wait_recv()

    each(1, S, returned)
    rows = back[...].astype(F32).reshape(S * R, CW).astype(BF16)
    for k in range(top):
        base = base + dot(picks[k], rows) * own_weights[k]
    out_ref[...] = base.astype(BF16)

    def close_keys(d):
        for copy in ag_copies(d) + fw_copies(d):
            copy.wait_send()

    for copy in own_copies:
        copy.wait_send()
    each(1, nz, close_keys)
    each(1, S, lambda d: di_copy(d).wait_send())
    each(1, S, lambda d: rt_copy(d).wait_send())

    def close(e):
        p_copy(e).wait_send()
        st_copy(e).wait_send()
        sh_copy(e).wait_send()
        rl_own(e).wait_send()
        each(1, S, lambda d: rl_copy(d, e).wait_send())
        each(0, S, lambda i: pd_copy(e, i).wait_send())

    each(1, T, close)


def local(
    S, T,
    wide_queries, narrow_queries, kv_latent, rope_key, latent_gain, wide_kv_weight, narrow_kv_weight,
    wide_out_weight, narrow_out_weight, residual, norm_gain, route_ids, route_weights,
    expert_gate, expert_up, expert_down, shared_gate, shared_up, shared_down,
):
    tok, D = residual.shape
    latent_dim = kv_latent.shape[1]
    top = route_ids.shape[1]
    local_experts = expert_gate.shape[0]
    cap = max(2, 3 * tok * top // (2 * S * local_experts))
    R = -(-local_experts * cap // 8) * 8
    CW = D // T

    vm = pl.BlockSpec(memory_space=pltpu.VMEM)
    hbm = pl.BlockSpec(memory_space=pl.ANY)
    weights = (
        wide_kv_weight, narrow_kv_weight, wide_out_weight, narrow_out_weight,
        expert_gate, expert_up, expert_down, shared_gate, shared_up, shared_down,
    )
    small = (
        wide_queries, narrow_queries, kv_latent, rope_key.T, latent_gain[None, :], residual,
        norm_gain[None, :], route_ids.T, route_weights.T,
    )
    V = pltpu.VMEM
    sem = pltpu.SemaphoreType.DMA
    ff = expert_gate.shape[2]
    scratch = [V(w.shape, w.dtype) for w in weights] + [
        V((tok, latent_dim), BF16),
        V((tok * ROPE_DIM // LANES, LANES), BF16),
        V((S, tok, latent_dim), BF16),
        V((S, tok * ROPE_DIM // LANES, LANES), BF16),
        V((T, tok, CW), BF16),
        V((T, tok, CW), BF16),
        V((T, tok, CW), BF16),
        V((S, R, CW), BF16),
        V((T, S, R, CW), BF16),
        V((2 * local_experts, S * R, ff), F32),
        V((T, tok, CW), BF16),
        V((T, tok, CW), BF16),
        V((T, S, R, CW), BF16),
        V((T, S, R, CW), BF16),
        V((S, R, CW), BF16),
        V((S, R, CW), BF16),
        sem((len(weights),)), sem((S,)), sem((S,)), sem((2 * S,)),
        sem((T,)), sem((T,)), sem((T,)), sem((T,)),
        sem((S,)), sem((S, T)), sem((T, S)), sem((T,)), sem((T,)),
        sem((T, S)), sem((T, S)), sem((S,)), sem((S,)),
    ]
    return pl.pallas_call(
        functools.partial(kernel, (S, T, R, cap)),
        out_shape=jax.ShapeDtypeStruct((tok, CW), BF16),
        in_specs=[vm] * len(small) + [hbm] * len(weights),
        out_specs=vm,
        scratch_shapes=scratch,
        compiler_params=pltpu.CompilerParams(
            collective_id=0, has_side_effects=True, vmem_limit_bytes=60 * 1024 * 1024
        ),
    )(*small, *weights)


def solution(mesh):
    placed = (
        P("sp", "tp"),
        P("sp", "tp"),
        P("sp", None),
        P("sp", None),
        P(),
        P(None, "tp"),
        P(None, "tp"),
        P("tp", None),
        P("tp", None),
        P("sp", None),
        P(),
        P("sp", None),
        P("sp", None),
        P("sp", None, "tp"),
        P("sp", None, "tp"),
        P("sp", "tp", None),
        P(None, "tp"),
        P(None, "tp"),
        P("tp", None),
    )
    return jax.shard_map(
        functools.partial(local, mesh.shape["sp"], mesh.shape["tp"]),
        mesh=mesh, in_specs=placed, out_specs=P("sp", "tp"), check_vma=False,
    )
```
